128 devices in a mesh: sp: 16 (over z, y), tp: 8 (over x, core).
Axes of the slice: x: 4, y: 4, z: 4, core: 2. Of those that a mesh axis runs over, the one named last changes fastest.
Arguments:
- stream: bfloat16 [32768, 4096], P('sp', 'tp'), may hold values from -18 to 18
- doc_ids: int32 [32768], P('sp'), may hold values from 0 to 3, never falling along the last dimension, each value on 1 to 12288 neighbouring positions
- norm_gain: bfloat16 [3, 4096], replicated, may hold values from 0.099609375 to 1.8984375
- proj_in: bfloat16 [3, 4096, 1024], P(None, 'tp', 'sp'), may hold values from -0.09375 to 0.09375
- mix_pool: bfloat16 [3, 8, 128, 128], replicated, may hold values from -0.5 to 0.5
- pool_gain: bfloat16 [3, 1024], replicated, may hold values from 0.099609375 to 1.8984375
- proj_out: bfloat16 [3, 1024, 4096], P(None, 'sp', 'tp'), may hold values from -0.1875 to 0.1875
Outputs:
- stream_out: bfloat16 [32768, 4096], P('sp', 'tp')
The draws below stay inside these ranges and needn't reach their ends.
Inputs may be any that keep to these rules, and one draw needn't show every extreme that they name: `doc_ids`: document numbers never fall along the sequence; each document holds 1 to 12288 positions, one exactly that many.
All inputs are finite; a program needn't handle non-finite values.
Results may differ from the reference program's by a relative error of at most 0.02.
Values may be sent and summed in bfloat16 or wider, within the bound.
No kernel may reach another device: no remote copies, remote signals or barrier semaphores. Data moves between devices by JAX's collectives and lax.ppermute only.
A program may use at most 64 MiB of HBM per device.

```python
import math
import jax
import jax.numpy as jnp
import numpy as np
from jax import lax

D = 4096
POOL = 1024
GROUP = 128
LAYERS = 3
TOK = 2048
GROUPS = 8
TOKENS = 32768
DOCS = 4
N_TP = 8


def draw_stream(key, part):
    key_base = jax.random.fold_in(key, 11)
    key_cols = jax.random.fold_in(key, 12)
    column_scale = jnp.exp(jax.random.uniform(key_cols, (32,), jnp.float32, -1.1, 1.1))
    column_scale = jnp.repeat(column_scale, D // 32)
    base = jnp.clip(jax.random.normal(key_base, (TOKENS, D), jnp.float32), -6.0, 6.0)
    values = jnp.clip(base * column_scale[None, :], -18.0, 18.0)
    return values.astype(jnp.bfloat16)


def block_scale(own_key, shape, pieces, low, high):
    level, own = 1.0, jax.random.fold_in(own_key, 6)
    for position, blocks in pieces:
        steps = jnp.exp(jax.random.uniform(jax.random.fold_in(own, position), (blocks,), jnp.float32, low / len(pieces), high / len(pieces)))
        level = level * jnp.repeat(steps, shape[position] // blocks).reshape([-1 if axis == position else 1 for axis in range(len(shape))])
    return level


def split_up(count, total, limit, lean):
    portions = [(1 << 20) // math.isqrt(rank ** lean) + 1 for rank in range(2, count + 1)]
    spare, given = total - limit - (count - 1), [1] * (count - 1)
    while spare > 0:
        movable = [i for i in range(count - 1) if given[i] < limit]
        whole, left = sum([portions[i] for i in movable]), spare
        for i in movable:
            more = min(limit - given[i], max(1, left * portions[i] // whole), spare)
            given[i] = given[i] + more
            spare = spare - more
    return np.array([limit] + given)


def ragged(rng, count, total, limit, slope):
    if count == 2:
        one = jax.random.randint(rng, (), max(1, total - limit), min(limit, total - 1) + 1)
        return jnp.stack([one, total - one])
    lengths = jnp.asarray(split_up(count, total, limit, slope), jnp.int32)
    twos = (count - 1) // 2
    source_of, receiver = lengths[1:1 + 2 * twos:2], lengths[2:2 + 2 * twos:2]
    room = jnp.minimum(source_of - 1, limit - receiver)
    passed = jax.random.randint(jax.random.fold_in(rng, 1), (twos,), 0, 1 << 20) % (room + 1)
    lengths = lengths.at[1:1 + 2 * twos:2].set(source_of - passed).at[2:2 + 2 * twos:2].set(receiver + passed)
    return lengths[jax.random.permutation(jax.random.fold_in(rng, 2), count)]


def normal_values(rng, dims, deviation, bound, shards=(), held_as=jnp.bfloat16):
    entries = jax.random.normal(rng, dims, jnp.float32) * deviation
    if len(shards) > 0:
        entries = block_scale(rng, dims, shards, -0.22, 0.18) * entries
    return jnp.clip(entries, min=-bound, max=bound).astype(held_as)


def setup_inputs(seed: int = 0) -> dict:
    key_of = jax.random.split(jax.random.key(seed), 8)
    return {
        "stream": draw_stream(jax.random.fold_in(key_of[7], 71), 0),
        "doc_ids": jnp.searchsorted(jnp.cumsum(ragged(key_of[1], DOCS, TOKENS, 6 * TOK, 1)), jnp.arange(TOKENS), side="right").astype(jnp.int32),
        "norm_gain": jnp.clip(1.0 + 0.18 * jax.random.normal(key_of[2], (LAYERS, D), jnp.float32), 0.099609375, 1.8984375).astype(jnp.bfloat16),
        "proj_in": normal_values(key_of[3], (LAYERS, D, POOL), D ** -0.5, 0.09375, ((1, 8), (2, 16))),
        "mix_pool": normal_values(key_of[4], (LAYERS, GROUPS, GROUP, GROUP), GROUP ** -0.5, 0.5),
        "pool_gain": jnp.clip(1.0 + 0.18 * jax.random.normal(key_of[5], (LAYERS, POOL), jnp.float32), 0.099609375, 1.8984375).astype(jnp.bfloat16),
        "proj_out": normal_values(key_of[6], (LAYERS, POOL, D), POOL ** -0.5, 0.1875, ((1, 16), (2, 8))),
    }


epsilon = 1e-06
span_reach = 15

def span_pool(padded, labels, widths):
    kept = padded.shape[0] - span_reach
    own_label = labels[span_reach:]
    summed = jnp.zeros((kept, padded.shape[1]), jnp.float32)
    counted = jnp.zeros((kept, padded.shape[1]), jnp.float32)
    for offset in range(span_reach + 1):
        first = span_reach - offset
        member = (labels[first:first + kept] == own_label)[:, None] & (offset < widths)[None, :]
        factor = member.astype(jnp.float32)
        summed = summed + padded[first:first + kept] * factor
        counted = counted + factor
    return summed / counted - padded[span_reach:]

def reference(stream, doc_ids, norm_gain, proj_in, mix_pool, pool_gain, proj_out):
    hidden = stream
    labels = (doc_ids + 1).astype(jnp.int32)
    tags = jnp.concatenate([jnp.zeros((span_reach,), jnp.int32), labels])
    channel = jnp.arange(POOL, dtype=jnp.int32)
    widths = jnp.left_shift(jnp.int32(2), channel // GROUP % 4)
    block = D // N_TP
    for layer in range(LAYERS):
        wide = hidden.astype(jnp.float32)
        scale_rows = lax.rsqrt(lax.optimization_barrier(jnp.mean(wide * wide, axis=1)) + epsilon)
        gained = (wide * norm_gain[layer].astype(jnp.float32)[None, :]).astype(jnp.bfloat16)
        summed_in = jnp.zeros((hidden.shape[0], POOL), jnp.float32)
        for piece in range(N_TP):
            partial_value = jnp.dot(gained[:, piece * block:(piece + 1) * block], proj_in[layer, piece * block:(piece + 1) * block], preferred_element_type=jnp.float32)
            summed_in = summed_in + lax.optimization_barrier(partial_value.astype(jnp.bfloat16)).astype(jnp.float32)
        mixed_in = (summed_in * scale_rows[:, None]).astype(jnp.bfloat16)
        padded = jnp.concatenate([jnp.zeros((span_reach, POOL), jnp.float32), mixed_in.astype(jnp.float32)])
        pooled = span_pool(padded, tags, widths).astype(jnp.bfloat16)
        grouped = pooled.reshape(hidden.shape[0], GROUPS, GROUP).astype(jnp.float32)
        blended = jnp.einsum('tgc,gcd->tgd', grouped, mix_pool[layer].astype(jnp.float32)).reshape(hidden.shape[0], POOL)
        mixed = (blended * pool_gain[layer].astype(jnp.float32)[None, :]).astype(jnp.bfloat16)
        update = jnp.dot(mixed, proj_out[layer], preferred_element_type=jnp.float32)
        hidden = (wide + update).astype(jnp.bfloat16)
    return hidden
```

```python
import functools

import jax
import jax.numpy as jnp
from jax import lax
from jax.experimental import pallas as pl
from jax.experimental.pallas import tpu as pltpu
from jax.sharding import Mesh, PartitionSpec as P


epsilon = 1e-06
HALO = 64
TAIL = 16
SEQ = ("z", "y")
F32 = jnp.float32
BF16 = jnp.bfloat16


def params(*semantics):
    return pltpu.CompilerParams(
        dimension_semantics=semantics or None, vmem_limit_bytes=40 * 1024 * 1024
    )


def nt_dot(a, b):
    return lax.dot_general(a, b, (((1,), (1,)), ((), ())), preferred_element_type=F32)


def dot(a, b):
    return jnp.dot(a, b, preferred_element_type=F32)


def quarter_rows(index, k):
    return pl.ds(pl.multiple_of(index[k] * 256, 256), 256)


def project_body(index, own, other, gain, weight, keep, send):
    width = own.shape[1]
    first = (own[...].astype(F32) * gain[:, :width]).astype(BF16)
    second = (other[...].astype(F32) * gain[:, width:]).astype(BF16)
    for k in range(4):
        rows = quarter_rows(index, k)
        part = nt_dot(first, weight[rows, :width]) + nt_dot(second, weight[rows, width:])
        out = keep if k < 2 else send
        out[:, (k % 2) * 256 : (k % 2 + 1) * 256] = part.astype(BF16)


def project(index, own, other, gain, weight, blocks):
    rows, width = own.shape
    step = rows // blocks
    row_block = pl.BlockSpec((step, width), lambda i, s: (i, 0))
    half = weight.shape[0] // 2
    out_block = pl.BlockSpec((step, half), lambda i, s: (i, 0))
    return pl.pallas_call(
        project_body,
        grid_spec=pltpu.PrefetchScalarGridSpec(
            num_scalar_prefetch=1,
            grid=(blocks,),
            in_specs=[
                row_block,
                row_block,
                pl.BlockSpec(gain.shape, lambda i, s: (0, 0)),
                pl.BlockSpec(weight.shape, lambda i, s: (0, 0)),
            ],
            out_specs=[out_block, out_block],
        ),
        out_shape=[jax.ShapeDtypeStruct((rows, half), BF16)] * 2,
        compiler_params=params("arbitrary"),
        cost_estimate=pl.CostEstimate(
            flops=2 * rows * width * 2 * half * 2,
            bytes_accessed=8 * 1024 * 1024,
            transcendentals=0,
        ),
        name="project",
    )(index, own, other, gain, weight)


def pool_body(model_width, near, far, across, sq_own, sq_core, sq_pair, band, share, mix, gain, mixed):
    rows = near.shape[0]
    total = sq_own[...] + sq_core[...] + sq_pair[...]
    scale = lax.rsqrt(total * (1.0 / model_width) + epsilon)
    before = jnp.zeros((TAIL, 256), BF16)
    for start in range(0, rows, 128):
        size = min(128, rows - start)
        here = slice(start, start + size)
        turned = jnp.transpose(jnp.broadcast_to(scale[0:1, start : start + 128], (128, 128)))[:size]
        summed = near[here, :].astype(F32) + far[here, :].astype(F32) + across[here, :].astype(F32)
        z = (summed * jnp.concatenate([turned, turned], axis=1)).astype(BF16)
        window = jnp.concatenate([before, z], axis=0)
        before = z[size - TAIL :]
        for g in range(2):
            cols = slice(g * 128, (g + 1) * 128)
            sums = dot(band[g, here, : size + TAIL], window[:, cols])
            pooled = (sums * share[g, here, :] - z[:, cols].astype(F32)).astype(BF16)
            blended = dot(pooled, mix[g]) * gain[0:1, cols]
            mixed[here, cols] = blended.astype(BF16)


def pool(near, far, across, squares, band, share, mix, gain, model_width):
    rows = near.shape[0]
    left = pl.BlockSpec((rows, 256), lambda i: (0, 0))
    whole = lambda a: pl.BlockSpec(a.shape, lambda i, n=a.ndim: (0,) * n)
    return pl.pallas_call(
        functools.partial(pool_body, model_width),
        grid=(1,),
        in_specs=[left, left, left] + [whole(a) for a in (*squares, band, share, mix, gain)],
        out_specs=left,
        out_shape=jax.ShapeDtypeStruct((rows, 256), BF16),
        compiler_params=params("arbitrary"),
        cost_estimate=pl.CostEstimate(
            flops=2 * rows * 256 * 1024, bytes_accessed=4 * 1024 * 1024, transcendentals=0
        ),
        name="pool",
    )(near, far, across, *squares, band, share, mix, gain)


def update_body(index, m0, m1, m2, m3, own, other, weight, new_own, new_other, squares):
    width = own.shape[1]
    total = None
    for k, part in enumerate((m0, m1, m2, m3)):
        term = dot(part[...], weight[quarter_rows(index, k), :])
        total = term if total is None else total + term
    first = (own[...].astype(F32) + total[:, :width]).astype(BF16)
    second = (other[...].astype(F32) + total[:, width:]).astype(BF16)
    new_own[...] = first
    new_other[...] = second
    if squares is not None:
        fold = first.astype(F32) ** 2 + second.astype(F32) ** 2
        ones = jnp.ones((8, width), BF16)
        high = fold.astype(BF16)
        low = (fold - high.astype(F32)).astype(BF16)
        squares[0] = nt_dot(ones, high) + nt_dot(ones, low)


def update(index, parts, own, other, weight, blocks):
    rows, width = own.shape
    step = rows // blocks
    row_block = pl.BlockSpec((step, width), lambda i, s: (i, 0))
    part_block = pl.BlockSpec((step, 256), lambda i, s: (i, 0))
    shape = jax.ShapeDtypeStruct((rows, width), BF16)
    return pl.pallas_call(
        update_body,
        grid_spec=pltpu.PrefetchScalarGridSpec(
            num_scalar_prefetch=1,
            grid=(blocks,),
            in_specs=[part_block] * 4
            + [row_block] * 2
            + [pl.BlockSpec(weight.shape, lambda i, s: (0, 0))],
            out_specs=[row_block] * 2 + [pl.BlockSpec((1, 8, step), lambda i, s: (i, 0, 0))],
        ),
        out_shape=[shape, shape, jax.ShapeDtypeStruct((blocks, 8, step), F32)],
        compiler_params=params("arbitrary"),
        cost_estimate=pl.CostEstimate(
            flops=2 * rows * 1024 * width * 2, bytes_accessed=10 * 1024 * 1024, transcendentals=0
        ),
        name="update",
    )(index, *parts, own, other, weight)


def along_sequence(value, count):
    return lax.ppermute(value, SEQ, [(i, i + 1) for i in range(count - 1)])


def body(stream, doc_ids, norm_gain, proj_in, mix_pool, pool_gain, proj_out):
    layers = proj_in.shape[0]
    tokens, width = stream.shape
    model_width = norm_gain.shape[1]
    places = lax.axis_size(SEQ)
    x, c = lax.axis_index("x"), lax.axis_index("c")
    late, p = x // 2, x % 2
    flip = [(i, 3 - i) for i in range(4)]
    pair = [(i, i ^ 1) for i in range(4)]
    swap = [(0, 1), (1, 0)]
    half = tokens // 2
    rows = half + HALO

    weights = jnp.stack([jnp.swapaxes(proj_in, 1, 2), proj_out], axis=1).reshape(
        2 * layers, -1, width
    )

    def everyone(shard):
        pieces = lax.all_to_all(
            jnp.broadcast_to(shard[None], (places, *shard.shape)), SEQ, 0, 0, tiled=True
        )
        return pieces.reshape(-1, shard.shape[-1])

    def both_blocks(shards):
        return jnp.concatenate([shards, lax.ppermute(shards, "x", flip)], axis=-1)

    shards = [both_blocks(weights[i]) for i in range(2 * layers)]
    full = [everyone(s) for s in shards]

    extended = jnp.concatenate([along_sequence(stream[-HALO:], places), stream], axis=0)
    labels = (doc_ids + 1).astype(jnp.int32)
    labels = jnp.concatenate([along_sequence(labels[-HALO:], places), labels])
    own = lax.dynamic_slice_in_dim(extended, late * half, rows)
    away = lax.dynamic_slice_in_dim(extended, (1 - late) * half, rows)
    labels = lax.dynamic_slice_in_dim(labels, late * half, rows)
    other = lax.ppermute(away, "x", flip)

    quarters = jnp.stack([2 * c + p, 2 * c + 1 - p, 2 * (1 - c) + p, 2 * (1 - c) + 1 - p]).astype(
        jnp.int32
    )
    group = 2 * (2 * c + p)

    blocks = -(-rows // 128)
    padded = jnp.pad(labels, (TAIL, blocks * 128 - rows), constant_values=-1)
    sources = jnp.stack([padded[128 * b : 128 * b + 128 + TAIL] for b in range(blocks)])
    targets = padded[TAIL:].reshape(blocks, 128, 1)
    delta = (
        lax.broadcasted_iota(jnp.int32, (128, 128 + TAIL), 0)
        + TAIL
        - lax.broadcasted_iota(jnp.int32, (128, 128 + TAIL), 1)
    )
    member = (sources[:, None, :] == targets) & (delta >= 0)[None]
    bands, shares = [], []
    for g in range(2):
        window = jnp.left_shift(2, (group + g) % 4)
        band = (member & (delta < window)[None]).reshape(blocks * 128, -1)[:rows]
        count = jnp.sum(band.astype(F32), axis=1, keepdims=True)
        bands.append(band.astype(BF16))
        shares.append(jnp.broadcast_to(1.0 / count, (rows, 128)))
    band, share = jnp.stack(bands), jnp.stack(shares)

    def in_lanes(squares):
        return jnp.pad(squares, (0, blocks * 128 - rows))[None]

    first, second = own.astype(F32), other.astype(F32)
    squares = jnp.sum(first * first, axis=1) + jnp.sum(second * second, axis=1)
    here, there = (x * 2 + c) * width, ((3 - x) * 2 + c) * width
    for layer in range(layers):
        gain = jnp.concatenate(
            [lax.dynamic_slice_in_dim(norm_gain[layer], at, width) for at in (here, there)]
        ).astype(F32)[None]
        keep, send = project(index=quarters, own=own, other=other, gain=gain, weight=full[2 * layer], blocks=4)
        sq_own = in_lanes(squares)
        sq_core = lax.ppermute(sq_own, "c", swap)
        sq_pair = lax.ppermute(sq_own + sq_core, "x", pair)
        core = lax.ppermute(send, "c", swap)
        partner = (keep[:, 256:].astype(F32) + core[:, 256:].astype(F32)).astype(BF16)
        across = lax.ppermute(partner, "x", pair)
        mix = lax.dynamic_slice_in_dim(mix_pool[layer], group, 2, 0)
        scale = lax.dynamic_slice_in_dim(pool_gain[layer], group * 128, 256).astype(F32)[None]
        mixed = pool(
            keep, core, across, (sq_own, sq_core, sq_pair), band, share, mix, scale, model_width
        )
        from_core = lax.ppermute(mixed, "c", swap)
        from_pair = lax.ppermute(mixed, "x", pair)
        from_both = lax.ppermute(from_pair, "c", swap)
        own, other, sq = update(
            quarters, (mixed, from_pair, from_core, from_both), own, other, full[2 * layer + 1], 4
        )
        squares = sq[:, 0, :].reshape(-1)
    own, away = own[HALO:], other[HALO:]
    back = lax.ppermute(away, "x", flip)
    out = jnp.zeros((tokens, width), BF16)
    out = lax.dynamic_update_slice_in_dim(out, own, late * half, 0)
    return lax.dynamic_update_slice_in_dim(out, back, (1 - late) * half, 0)


def solution(mesh):
    fine = Mesh(mesh.devices.reshape(4, 4, 4, 2), ("z", "y", "x", "c"))
    sp, tp = ("z", "y"), ("x", "c")
    in_specs = (P(sp, tp), P(sp), P(), P(None, tp, sp), P(), P(), P(None, sp, tp))
    return jax.shard_map(body, mesh=fine, in_specs=in_specs, out_specs=P(sp, tp), check_vma=False)
```

```python
import functools

import jax
import jax.numpy as jnp
from jax import lax
from jax.experimental import pallas as pl
from jax.experimental.pallas import tpu as pltpu
from jax.sharding import Mesh, PartitionSpec as P


epsilon = 1e-06
HALO = 64
TAIL = 16
EXTRA = 16
PIECES = 2
VMEM_LIMIT = 16 * 1024 * 1024
LANES = 1024
SEQ = ("z", "y")
F32 = jnp.float32
BF16 = jnp.bfloat16


def nt_dot(a, b):
    return lax.dot_general(a, b, (((1,), (1,)), ((), ())), preferred_element_type=F32)


def dot(a, b):
    return jnp.dot(a, b, preferred_element_type=F32)


def quarter_of(weight, at, index, k):
    return weight[pl.ds(index[k] * 4, 4), at].reshape(256, weight.shape[3])


def call(kernel, operands, shapes, flops, scalars=True, scratch=()):
    memory = pl.BlockSpec(memory_space=pltpu.VMEM)
    specs = [memory] * len(operands)
    if scalars:
        specs[0] = pl.BlockSpec(memory_space=pltpu.SMEM)
    return pl.pallas_call(
        kernel,
        in_specs=specs,
        out_specs=[memory] * len(shapes),
        out_shape=[jax.ShapeDtypeStruct(s, t) for s, t in shapes],
        scratch_shapes=list(scratch),
        compiler_params=pltpu.CompilerParams(vmem_limit_bytes=VMEM_LIMIT),
        cost_estimate=pl.CostEstimate(flops=flops, bytes_accessed=1024, transcendentals=0),
    )(*operands)


def packed(total, lanes):
    high = total.astype(BF16).astype(F32)
    low = total - high
    count = LANES // lanes
    row = lax.broadcasted_iota(jnp.int32, (EXTRA, lanes), 0)
    out = jnp.zeros((EXTRA, lanes), F32)
    for i in range(count):
        cols = slice(i * lanes, (i + 1) * lanes)
        out = jnp.where(row == i, high[:, cols], out)
        out = jnp.where(row == count + i, low[:, cols], out)
    return out.astype(BF16)


def unpacked(block):
    count = LANES // block.shape[1]
    value = block.astype(F32)
    return jnp.concatenate(
        [value[i : i + 1] + value[count + i : count + i + 1] for i in range(count)], axis=1
    )


def square_sums(wide, ones):
    fold = wide * wide
    high = fold.astype(BF16)
    low = (fold - high.astype(F32)).astype(BF16)
    return nt_dot(ones, high) + nt_dot(ones, low)


def over_pieces(rows, one):
    size = rows // PIECES
    for i in range(PIECES):
        one(i, slice(i * size, (i + 1) * size))


def project_piece(index, i, here, wide, gain, weight, at, keep, send, sums):
    sums[i] = square_sums(wide, jnp.ones((8, wide.shape[1]), BF16))
    gained = (wide * gain[...]).astype(BF16)
    for k in range(4):
        columns = jnp.concatenate([quarter_of(weight, j, index, k) for j in at], axis=1)
        part = nt_dot(gained, columns)
        out = keep if k < 2 else send
        out[here, (k % 2) * 256 : (k % 2 + 1) * 256] = part.astype(BF16)


def finish_squares(sums, rows, send, squares):
    parts = [sums[i] for i in range(PIECES)]
    total = jnp.concatenate(parts + [jnp.zeros((8, LANES - rows), F32)], axis=1)[0:1]
    send[rows : rows + EXTRA, :] = packed(total, send.shape[1])
    squares[...] = total


def project_body(index, mine, away, gain, weight, keep, send, squares, sums):
    rows = mine.shape[0]
    for half, source in enumerate((mine, away)):

        def one(i, here):
            wide = source[here, :].astype(F32)
            project_piece(
                index, i, here, wide, gain, weight, (0,), keep.at[half], send.at[half], sums
            )

        over_pieces(rows, one)
        finish_squares(sums, rows, send.at[half], squares.at[half])


def updated(index, here, parts, old, weight, at):
    total = old[here, :].astype(F32)
    for k, part in enumerate(parts):
        total = total + dot(part[here, :], quarter_of(weight, at, index, k))
    return total.astype(BF16)


def step_body(
    at, index, m0, m1, m2, m3, own, other, gain, weight, new_own, new_other, keep, send, squares, sums
):
    def one(i, here):
        first = updated(index, here, (m0, m1, m2, m3), own, weight, at)
        second = updated(index, here, (m0, m1, m2, m3), other, weight, at + 5)
        new_own[here, :] = first
        new_other[here, :] = second
        wide = jnp.concatenate([first, second], axis=1).astype(F32)
        project_piece(index, i, here, wide, gain, weight, (at + 1, at + 6), keep, send, sums)

    over_pieces(own.shape[0], one)
    finish_squares(sums, own.shape[0], send, squares)


def last_body(at, skip, index, m0, m1, m2, m3, a0, a1, a2, a3, own, away, weight, out, out_away):
    size = out.shape[0] // PIECES
    for i in range(PIECES):
        there = slice(i * size, (i + 1) * size)
        here = slice(i * size + skip, (i + 1) * size + skip)
        out[there, :] = updated(index, here, (m0, m1, m2, m3), own, weight, at)
        out_away[there, :] = updated(index, here, (a0, a1, a2, a3), away, weight, at)


def merge_body(keep, core, squares, partner, chip):
    rows = keep.shape[0]
    partner[:rows, :] = (
        keep[:, 256:].astype(F32) + core[:rows, 256:].astype(F32)
    ).astype(BF16)
    total = squares[...] + unpacked(core[rows : rows + EXTRA, :])
    chip[...] = total
    partner[rows : rows + EXTRA, :] = packed(total, 256)


def scatter_body(keep, core, squares, to_pair, to_flip, to_cross, chip):
    rows = keep.shape[1]
    extra = slice(rows, rows + EXTRA)
    totals = [squares[half] + unpacked(core[half, extra, :]) for half in range(2)]
    chip[...] = totals[0]
    for out, half, first in ((to_pair, 0, 256), (to_flip, 1, 256), (to_cross, 1, 0)):
        cols = slice(first, first + 256)
        out[:rows, :] = (
            keep[half, :, cols].astype(F32) + core[half, :rows, cols].astype(F32)
        ).astype(BF16)
        out[extra, :] = packed(totals[half], 256)


def pool_rows(model_width, near, far, across, chip, tail, band, share, mix, gain, mixed, new_tail):
    rows = mixed.shape[0]
    total = chip[...]
    for part in across:
        total = total + unpacked(part[rows : rows + EXTRA, :])
    scale = lax.rsqrt(total * (1.0 / model_width) + epsilon)
    before = tail[...]
    for start in range(0, rows, 128):
        size = min(128, rows - start)
        here = slice(start, start + size)
        turned = jnp.transpose(jnp.broadcast_to(scale[:, start : start + 128], (128, 128)))[:size]
        summed = near(here).astype(F32) + far(here).astype(F32)
        for part in across:
            summed = summed + part[here, :].astype(F32)
        z = (summed * jnp.concatenate([turned, turned], axis=1)).astype(BF16)
        window = jnp.concatenate([before, z], axis=0)
        before = z[size - TAIL :]
        for g in range(2):
            cols = slice(g * 128, (g + 1) * 128)
            sums = dot(band[g, here, : size + TAIL], window[:, cols])
            pooled = (sums * share[g, here, :] - z[:, cols].astype(F32)).astype(BF16)
            blended = dot(pooled, mix[g]) * gain[0:1, cols]
            mixed[here, cols] = blended.astype(BF16)
    new_tail[...] = before


def pool_body(model_width, near, far, across, *rest):
    pool_rows(
        model_width, lambda r: near[r, :256], lambda r: far[r, :256], (across,), *rest
    )


def pool_first_body(model_width, near, far, across, flipped, crossed, *rest):
    pool_rows(
        model_width,
        lambda r: near[0, r, :256],
        lambda r: far[0, r, :256],
        (across, flipped, crossed),
        *rest,
    )


def along_sequence(value, count):
    return lax.ppermute(value, SEQ, [(i, i + 1) for i in range(count - 1)])


def membership(padded, start, rows, group):
    blocks = -(-rows // 128)
    padded = jnp.pad(padded, (0, 128), constant_values=-1)
    sources = jnp.stack(
        [padded[start + 128 * b : start + 128 * b + 128 + TAIL] for b in range(blocks)]
    )
    targets = padded[start + TAIL : start + TAIL + 128 * blocks].reshape(blocks, 128, 1)
    delta = (
        lax.broadcasted_iota(jnp.int32, (128, 128 + TAIL), 0)
        + TAIL
        - lax.broadcasted_iota(jnp.int32, (128, 128 + TAIL), 1)
    )
    member = (sources[:, None, :] == targets) & (delta >= 0)[None]
    bands, shares = [], []
    for g in range(2):
        window = jnp.left_shift(2, (group + g) % 4)
        band = (member & (delta < window)[None]).reshape(blocks * 128, -1)[:rows]
        count = jnp.sum(band.astype(F32), axis=1, keepdims=True)
        bands.append(band.astype(BF16))
        shares.append(jnp.broadcast_to(1.0 / count, (rows, 128)))
    return jnp.stack(bands), jnp.stack(shares)


def layers_body(stream, doc_ids, norm_gain, proj_in, mix_pool, pool_gain, proj_out):
    layers = proj_in.shape[0]
    tokens, width = stream.shape
    model_width = norm_gain.shape[1]
    places = lax.axis_size(SEQ)
    x, c = lax.axis_index("x"), lax.axis_index("c")
    late, p = x // 2, x % 2
    flip = [(i, 3 - i) for i in range(4)]
    pair = [(i, i ^ 1) for i in range(4)]
    swap = [(0, 1), (1, 0)]
    half = tokens // 2
    rows = half + HALO
    split = half // 2 + HALO
    streams = [(0, split), (split, rows)]

    turned = jnp.swapaxes(proj_in, 1, 2)
    chain = [turned[0]]
    for layer in range(layers):
        chain.append(proj_out[layer])
        if layer + 1 < layers:
            chain.append(turned[layer + 1])

    def spread(shards):
        return jnp.broadcast_to(shards[None], (places, *shards.shape))

    def everyone(copies):
        return lax.all_to_all(copies, SEQ, 0, 0, tiled=True)

    labels_of = (doc_ids + 1).astype(jnp.int32)
    marks = jnp.pad(
        labels_of[-HALO:].astype(BF16)[None], ((0, EXTRA - 1), (0, width - HALO))
    )
    lead = along_sequence(jnp.concatenate([stream[-HALO:], marks]), places)
    w_first = everyone(spread(chain[0][None]))
    lead_labels = lead[HALO, :HALO].astype(jnp.int32)
    lead = lead[:HALO]
    middle = stream[half - HALO : half]
    middle_labels = labels_of[half - HALO : half]
    own_lead = jnp.where(late == 1, middle, lead)
    other_lead = jnp.where(late == 1, lead, middle)
    labels = jnp.concatenate(
        [
            jnp.where(late == 1, middle_labels, lead_labels),
            lax.dynamic_slice_in_dim(labels_of, late * half, half),
        ]
    )
    quarter = half // 2

    def rows_at(side, s):
        return lax.dynamic_slice_in_dim(stream, side * half + s * quarter, quarter)

    own = [jnp.concatenate([own_lead, rows_at(late, 0)]), rows_at(late, 1)]
    away = [jnp.concatenate([other_lead, rows_at(1 - late, 0)]), rows_at(1 - late, 1)]
    mine = jnp.stack(chain[1:])
    theirs = lax.ppermute(mine[:4], "x", flip)
    other = []
    for s in range(2):
        other.append(lax.ppermute(away[s], "x", flip))
    w_rest = lax.all_gather(jnp.concatenate([mine, theirs]), SEQ, axis=0, tiled=False)

    quarters = jnp.stack([2 * c + p, 2 * c + 1 - p, 2 * (1 - c) + p, 2 * (1 - c) + 1 - p]).astype(
        jnp.int32
    )
    group = 2 * (2 * c + p)
    padded = jnp.pad(labels, (TAIL, 0), constant_values=-1)
    bands = [membership(padded, lo, hi - lo, group) for lo, hi in streams]

    here, there = (x * 2 + c) * width, ((3 - x) * 2 + c) * width

    def gain_of(layer):
        return jnp.concatenate(
            [lax.dynamic_slice_in_dim(norm_gain[layer], at, width) for at in (here, there)]
        ).astype(F32)[None]

    def sent_shapes(n):
        return [((n, 512), BF16), ((n + EXTRA, 512), BF16), ((1, LANES), F32)]

    def sums_of(n):
        return [pltpu.VMEM((PIECES, 8, n // PIECES), F32)]

    gains = [gain_of(layer) for layer in range(layers)]
    partial, sends, crossed = [], [], []
    for s, (lo, hi) in enumerate(streams):
        n = hi - lo
        partial.append(
            call(
                project_body,
                (quarters, own[s], away[s], gains[0][:, :width], w_first),
                [((2, *shape), kind) for shape, kind in sent_shapes(n)],
                2 * n * 1024 * 1024,
                scratch=sums_of(n),
            )
        )
        sends.append(lax.ppermute(partial[s][1], "c", swap))
    cross = [(i, (i + 2) % 4) for i in range(4)]
    for layer in range(layers):
        mix = lax.dynamic_slice_in_dim(mix_pool[layer], group, 2, 0)
        scale = lax.dynamic_slice_in_dim(pool_gain[layer], group * 128, 256).astype(F32)[None]
        last = layer + 1 == layers
        tail = jnp.zeros((TAIL, 256), BF16)
        merged, parts, back = [], [], []
        for s, (lo, hi) in enumerate(streams):
            n = hi - lo
            keep, _, squares = partial[s]
            message = ((n + EXTRA, 256), BF16)
            routes = (pair, flip, cross) if layer == 0 else (pair,)
            *messages, chip = call(
                scatter_body if layer == 0 else merge_body,
                (keep, sends[s], squares),
                [message] * len(routes) + [((1, LANES), F32)],
                n * 256,
                scalars=False,
            )
            across = [lax.ppermute(value, "x", route) for value, route in zip(messages, routes)]
            merged.append((keep, sends[s], *across, chip))
        for s, (lo, hi) in enumerate(streams):
            n = hi - lo
            band, share = bands[s]
            mixed, tail = call(
                functools.partial(pool_first_body if layer == 0 else pool_body, model_width),
                (*merged[s], tail, band, share, mix, scale),
                [((n, 256), BF16), ((TAIL, 256), BF16)],
                2 * n * 256 * 1024,
                scalars=False,
            )
            from_core = lax.ppermute(mixed, "c", swap)
            came = [
                lax.ppermute(mixed, "x", route)
                for route in ((pair, cross, flip) if last else (pair,))
            ]
            came_core = [lax.ppermute(value, "c", swap) for value in came]
            ours = (mixed, came[0], from_core, came_core[0])
            if last:
                ours = (*ours, *came[1:], *came_core[1:])
            parts.append(ours)
        for s, (lo, hi) in enumerate(streams):
            n = hi - lo
            if not last:
                own[s], other[s], *partial[s] = call(
                    functools.partial(step_body, 2 * layer),
                    (quarters, *parts[s], own[s], other[s], gains[layer + 1], w_rest),
                    [((n, width), BF16)] * 2 + sent_shapes(n),
                    4 * n * 1024 * 1024,
                    scratch=sums_of(n),
                )
            else:
                skip = HALO if s == 0 else 0
                own[s], back_rows = call(
                    functools.partial(last_body, 4, skip),
                    (quarters, *parts[s], own[s], crossed[s], w_rest),
                    [((n - skip, width), BF16)] * 2,
                    2 * n * 1024 * 1024,
                )
                back.append(back_rows)
            if not last:
                sends[s] = lax.ppermute(partial[s][1], "c", swap)
            if layer + 2 == layers:
                crossed.append(lax.ppermute(other[s], "x", flip))
    out = jnp.zeros((tokens, width), BF16)
    place = 0
    for s in range(2):
        out = lax.dynamic_update_slice_in_dim(out, own[s], late * half + place, 0)
        out = lax.dynamic_update_slice_in_dim(out, back[s], (1 - late) * half + place, 0)
        place += own[s].shape[0]
    return out


def solution(mesh):
    fine = Mesh(mesh.devices.reshape(4, 4, 4, 2), ("z", "y", "x", "c"))
    sp, tp = ("z", "y"), ("x", "c")
    in_specs = (P(sp, tp), P(sp), P(), P(None, tp, sp), P(), P(), P(None, sp, tp))
    return jax.shard_map(layers_body, mesh=fine, in_specs=in_specs, out_specs=P(sp, tp), check_vma=False)
```

```python
import functools

import jax
import jax.numpy as jnp
from jax import lax
from jax.experimental import pallas as pl
from jax.experimental.pallas import tpu as pltpu
from jax.sharding import Mesh, PartitionSpec as P


epsilon = 1e-06
HALO = 64
TAIL = 16
EXTRA = 16
PIECES = 1
VMEM_LIMIT = 16 * 1024 * 1024
LANES = 1024
SEQ = ("z", "y")
F32 = jnp.float32
BF16 = jnp.bfloat16


def nt_dot(a, b):
    return lax.dot_general(a, b, (((1,), (1,)), ((), ())), preferred_element_type=F32)


def dot(a, b):
    return jnp.dot(a, b, preferred_element_type=F32)


def quarter_of(weight, at, index, k):
    return weight[pl.ds(index[k] * 4, 4), at].reshape(256, weight.shape[3])


def call(kernel, operands, shapes, flops, scalars=True, scratch=()):
    memory = pl.BlockSpec(memory_space=pltpu.VMEM)
    specs = [memory] * len(operands)
    if scalars:
        specs[0] = pl.BlockSpec(memory_space=pltpu.SMEM)
    return pl.pallas_call(
        kernel,
        in_specs=specs,
        out_specs=[memory] * len(shapes),
        out_shape=[jax.ShapeDtypeStruct(s, t) for s, t in shapes],
        scratch_shapes=list(scratch),
        compiler_params=pltpu.CompilerParams(vmem_limit_bytes=VMEM_LIMIT),
        cost_estimate=pl.CostEstimate(flops=flops, bytes_accessed=1024, transcendentals=0),
    )(*operands)


def packed(total, lanes):
    high = total.astype(BF16).astype(F32)
    low = total - high
    count = LANES // lanes
    row = lax.broadcasted_iota(jnp.int32, (EXTRA, lanes), 0)
    out = jnp.zeros((EXTRA, lanes), F32)
    for i in range(count):
        cols = slice(i * lanes, (i + 1) * lanes)
        out = jnp.where(row == i, high[:, cols], out)
        out = jnp.where(row == count + i, low[:, cols], out)
    return out.astype(BF16)


def unpacked(block):
    count = LANES // block.shape[1]
    value = block.astype(F32)
    return jnp.concatenate(
        [value[i : i + 1] + value[count + i : count + i + 1] for i in range(count)], axis=1
    )


def square_sums(wide, ones):
    fold = wide * wide
    fold = sum(fold[:, i : i + 128] for i in range(0, fold.shape[1], 128))
    high = fold.astype(BF16)
    low = (fold - high.astype(F32)).astype(BF16)
    return nt_dot(ones, high) + nt_dot(ones, low)


def over_pieces(rows, one):
    size = rows // PIECES
    for i in range(PIECES):
        one(i, slice(i * size, (i + 1) * size))


def project_piece(index, i, here, wide, gain, weight, at, keep, send, sums):
    sums[i] = square_sums(wide, jnp.ones((8, 128), BF16))
    gained = (wide * gain[...]).astype(BF16)
    for k in range(4):
        columns = jnp.concatenate([quarter_of(weight, j, index, k) for j in at], axis=1)
        part = nt_dot(gained, columns)
        out = keep if k < 2 else send
        out[here, (k % 2) * 256 : (k % 2 + 1) * 256] = part.astype(BF16)


def finish_squares(sums, rows, send, squares):
    parts = [sums[i] for i in range(PIECES)]
    total = jnp.concatenate(parts + [jnp.zeros((8, LANES - rows), F32)], axis=1)[0:1]
    send[rows : rows + EXTRA, :] = packed(total, send.shape[1])
    squares[...] = total


def project_body(index, both, gain, weight, keep, send, squares, sums):
    rows = both.shape[1]

    def turn(half, carry):
        wide = both[half].astype(F32)
        project_piece(
            index, 0, slice(0, rows), wide, gain, weight, (0,), keep.at[half], send.at[half], sums
        )
        finish_squares(sums, rows, send.at[half], squares.at[half])
        return carry

    lax.fori_loop(0, 2, turn, 0)


def updated(index, here, parts, old, weight, at):
    total = old[here, :].astype(F32)
    for k, part in enumerate(parts):
        total = total + dot(part[here, :], quarter_of(weight, at, index, k))
    return total.astype(BF16)


def step_body(
    index, m0, m1, m2, m3, own, other, gain, weight, new_own, new_other, keep, send, squares, sums
):
    def one(i, here):
        first = updated(index, here, (m0, m1, m2, m3), own, weight, 0)
        second = updated(index, here, (m0, m1, m2, m3), other, weight, 1)
        new_own[here, :] = first
        new_other[here, :] = second
        wide = jnp.concatenate([first, second], axis=1).astype(F32)
        project_piece(index, i, here, wide, gain, weight, (2, 3), keep, send, sums)

    over_pieces(own.shape[0], one)
    finish_squares(sums, own.shape[0], send, squares)


def last_body(skip, index, m0, m1, m2, m3, own, other, weight, out, out_other):
    here = slice(skip, own.shape[0])
    out[...] = updated(index, here, (m0, m1, m2, m3), own, weight, 0)
    out_other[...] = updated(index, here, (m0, m1, m2, m3), other, weight, 1)


def merge_body(keep, core, squares, partner, chip):
    rows = keep.shape[0]
    partner[:rows, :] = (
        keep[:, 256:].astype(F32) + core[:rows, 256:].astype(F32)
    ).astype(BF16)
    total = squares[...] + unpacked(core[rows : rows + EXTRA, :])
    chip[...] = total
    partner[rows : rows + EXTRA, :] = packed(total, 256)


def scatter_body(keep, core, squares, to_pair, to_flip, to_cross, chip):
    rows = keep.shape[1]
    extra = slice(rows, rows + EXTRA)
    totals = [squares[half] + unpacked(core[half, extra, :]) for half in range(2)]
    chip[...] = totals[0]
    for out, half, first in ((to_pair, 0, 256), (to_flip, 1, 256), (to_cross, 1, 0)):
        cols = slice(first, first + 256)
        out[:rows, :] = (
            keep[half, :, cols].astype(F32) + core[half, :rows, cols].astype(F32)
        ).astype(BF16)
        out[extra, :] = packed(totals[half], 256)


def pool_rows(model_width, first, near, far, across, chip, tail, band, share, mix, gain, mixed, new_tail, scales):
    rows = mixed.shape[0]
    total = chip[...]
    for part in across:
        total = total + unpacked(part[rows : rows + EXTRA, :])
    scale = lax.rsqrt(total * (1.0 / model_width) + epsilon)
    for i in range(LANES // 128):
        scales[i] = scale[:, 128 * i : 128 * i + 128]

    def block(i, size, before):
        at = i * 128
        if looped:
            at = pl.multiple_of(at, 128)
        here, there = pl.ds(at, size), pl.ds(first + at, size)
        turned = jnp.transpose(jnp.broadcast_to(scales[i], (128, 128)))[:size]
        summed = near(here).astype(F32) + far(here).astype(F32)
        for part in across:
            summed = summed + part[here, :].astype(F32)
        z = (summed * jnp.concatenate([turned, turned], axis=1)).astype(BF16)
        window = jnp.concatenate([before, z], axis=0)
        for g in range(2):
            cols = slice(g * 128, (g + 1) * 128)
            sums = dot(band[g, there, : size + TAIL], window[:, cols])
            pooled = (sums * share[g, there, :] - z[:, cols].astype(F32)).astype(BF16)
            blended = dot(pooled, mix[g]) * gain[0:1, cols]
            mixed[here, cols] = blended.astype(BF16)
        return z[size - TAIL :]

    whole = rows // 128
    looped = len(across) > 1 or rows % 128 > 0
    before = tail[...]
    if looped:
        before = lax.fori_loop(0, whole, lambda i, carry: block(i, 128, carry), before)
        looped = False
    else:
        for i in range(whole):
            before = block(i, 128, before)
    if rows > whole * 128:
        before = block(whole, rows - whole * 128, before)
    new_tail[...] = before


def pool_body(model_width, first, near, far, across, *rest):
    pool_rows(
        model_width, first, lambda r: near[r, :256], lambda r: far[r, :256], (across,), *rest
    )


def pool_first_body(model_width, first, near, far, across, flipped, crossed, *rest):
    pool_rows(
        model_width,
        first,
        lambda r: near[0, r, :256],
        lambda r: far[0, r, :256],
        (across, flipped, crossed),
        *rest,
    )


def prepare_body(proj_in, proj_out, opening, mine):
    size = proj_in.shape[2]
    row = lax.broadcasted_iota(jnp.int32, (size, size), 0)
    eye = (row == lax.broadcasted_iota(jnp.int32, (size, size), 1)).astype(BF16)
    opening[...] = nt_dot(eye, proj_in[0]).astype(BF16)
    layers = proj_in.shape[0]
    for layer in range(layers):
        mine[2 * layer] = proj_out[layer]
        if layer + 1 < layers:
            mine[2 * layer + 1] = nt_dot(eye, proj_in[layer + 1]).astype(BF16)


def arrange_body(mine, theirs, out):
    for i in range(mine.shape[0]):
        out[2 * i] = mine[i]
        out[2 * i + 1] = theirs[i]


def along_sequence(value, count):
    return lax.ppermute(value, SEQ, [(i, i + 1) for i in range(count - 1)])


def membership(padded, start, rows, group):
    blocks = -(-rows // 128)
    padded = jnp.pad(padded, (0, 128), constant_values=-1)
    sources = jnp.stack(
        [padded[start + 128 * b : start + 128 * b + 128 + TAIL] for b in range(blocks)]
    )
    targets = padded[start + TAIL : start + TAIL + 128 * blocks].reshape(blocks, 128, 1)
    delta = (
        lax.broadcasted_iota(jnp.int32, (128, 128 + TAIL), 0)
        + TAIL
        - lax.broadcasted_iota(jnp.int32, (128, 128 + TAIL), 1)
    )
    member = (sources[:, None, :] == targets) & (delta >= 0)[None]
    bands, shares = [], []
    for g in range(2):
        window = jnp.left_shift(2, (group + g) % 4)
        band = (member & (delta < window)[None]).reshape(blocks * 128, -1)[:rows]
        count = jnp.sum(band.astype(F32), axis=1, keepdims=True)
        bands.append(band.astype(BF16))
        shares.append(jnp.broadcast_to(1.0 / count, (rows, 128)))
    return jnp.stack(bands), jnp.stack(shares)


def layers_body(stream, doc_ids, norm_gain, proj_in, mix_pool, pool_gain, proj_out):
    layers = proj_in.shape[0]
    tokens, width = stream.shape
    model_width = norm_gain.shape[1]
    places = lax.axis_size(SEQ)
    x, c = lax.axis_index("x"), lax.axis_index("c")
    late, p = x // 2, x % 2
    flip = [(i, 3 - i) for i in range(4)]
    pair = [(i, i ^ 1) for i in range(4)]
    swap = [(0, 1), (1, 0)]
    half = tokens // 2
    rows = half + HALO
    split = half // 2
    streams = [(0, split), (split, rows)]

    shard = (proj_in.shape[2], width)
    opening, mine = call(
        prepare_body,
        (proj_in, proj_out),
        [(shard, BF16), ((2 * layers - 1, *shard), BF16)],
        1024,
        scalars=False,
    )

    def spread(shards):
        return jnp.broadcast_to(shards[None], (places, *shards.shape))

    def everyone(copies):
        return lax.all_to_all(copies, SEQ, 0, 0, tiled=True)

    labels_of = (doc_ids + 1).astype(jnp.int32)
    marks = jnp.pad(
        labels_of[-HALO:].astype(BF16)[None], ((0, EXTRA - 1), (0, width - HALO))
    )
    lead = along_sequence(jnp.concatenate([stream[-HALO:], marks]), places)
    w_first = everyone(spread(opening[None]))
    lead_labels = lead[HALO, :HALO].astype(jnp.int32)
    lead = lead[:HALO]
    middle = stream[half - HALO : half]
    middle_labels = labels_of[half - HALO : half]
    own_lead = jnp.where(late == 1, middle, lead)
    other_lead = jnp.where(late == 1, lead, middle)
    labels = jnp.concatenate(
        [
            jnp.where(late == 1, middle_labels, lead_labels),
            lax.dynamic_slice_in_dim(labels_of, late * half, half),
        ]
    )

    def rows_at(side, s):
        lo, hi = max(0, streams[s][0] - HALO), streams[s][1] - HALO
        return lax.dynamic_slice_in_dim(stream, side * half + lo, hi - lo)

    own = [jnp.concatenate([own_lead, rows_at(late, 0)]), rows_at(late, 1)]
    away = [jnp.concatenate([other_lead, rows_at(1 - late, 0)]), rows_at(1 - late, 1)]
    theirs = lax.ppermute(mine, "x", flip)
    other = []
    for s in range(2):
        other.append(lax.ppermute(away[s], "x", flip))
    arranged = call(
        arrange_body, (mine, theirs), [((4 * layers - 2, *shard), BF16)], 1024, scalars=False
    )[0]
    w_rest = lax.all_gather(arranged, SEQ, axis=0, tiled=False)

    quarters = jnp.stack([2 * c + p, 2 * c + 1 - p, 2 * (1 - c) + p, 2 * (1 - c) + 1 - p]).astype(
        jnp.int32
    )
    group = 2 * (2 * c + p)
    padded = jnp.pad(labels, (TAIL, 0), constant_values=-1)
    band, share = membership(padded, 0, rows, group)

    here, there = (x * 2 + c) * width, ((3 - x) * 2 + c) * width

    def gain_of(layer):
        return jnp.concatenate(
            [lax.dynamic_slice_in_dim(norm_gain[layer], at, width) for at in (here, there)]
        ).astype(F32)[None]

    def sent_shapes(n):
        return [((n, 512), BF16), ((n + EXTRA, 512), BF16), ((1, LANES), F32)]

    def sums_of(n):
        return [pltpu.VMEM((PIECES, 8, n // PIECES), F32)]

    gains = [gain_of(layer) for layer in range(layers)]
    partial, sends = [], []
    for s, (lo, hi) in enumerate(streams):
        n = hi - lo
        partial.append(
            call(
                project_body,
                (quarters, jnp.stack([own[s], away[s]]), gains[0][:, :width], w_first),
                [((2, *shape), kind) for shape, kind in sent_shapes(n)],
                2 * n * 1024 * 1024,
                scratch=sums_of(n),
            )
        )
        sends.append(lax.ppermute(partial[s][1], "c", swap))
    cross = [(i, (i + 2) % 4) for i in range(4)]
    for layer in range(layers):
        mix = lax.dynamic_slice_in_dim(mix_pool[layer], group, 2, 0)
        scale = lax.dynamic_slice_in_dim(pool_gain[layer], group * 128, 256).astype(F32)[None]
        last = layer + 1 == layers
        w_step = w_rest[:, 4 * layer : 4 * layer + 4]
        tail = jnp.zeros((TAIL, 256), BF16)
        merged, parts, back = [], [], []
        for s, (lo, hi) in enumerate(streams):
            n = hi - lo
            keep, _, squares = partial[s]
            message = ((n + EXTRA, 256), BF16)
            routes = (pair, flip, cross) if layer == 0 else (pair,)
            *messages, chip = call(
                scatter_body if layer == 0 else merge_body,
                (keep, sends[s], squares),
                [message] * len(routes) + [((1, LANES), F32)],
                n * 256,
                scalars=False,
            )
            across = [lax.ppermute(value, "x", route) for value, route in zip(messages, routes)]
            merged.append((keep, sends[s], *across, chip))
        for s, (lo, hi) in enumerate(streams):
            n = hi - lo
            mixed, tail = call(
                functools.partial(pool_first_body if layer == 0 else pool_body, model_width, lo),
                (*merged[s], tail, band, share, mix, scale),
                [((n, 256), BF16), ((TAIL, 256), BF16)],
                2 * n * 256 * 1024,
                scalars=False,
                scratch=[pltpu.VMEM((LANES // 128, 1, 128), F32)],
            )
            from_core = lax.ppermute(mixed, "c", swap)
            from_pair = lax.ppermute(mixed, "x", pair)
            from_both = lax.ppermute(from_pair, "c", swap)
            parts.append((mixed, from_pair, from_core, from_both))
        for s, (lo, hi) in enumerate(streams):
            n = hi - lo
            if not last:
                own[s], other[s], *partial[s] = call(
                    step_body,
                    (quarters, *parts[s], own[s], other[s], gains[layer + 1], w_step),
                    [((n, width), BF16)] * 2 + sent_shapes(n),
                    4 * n * 1024 * 1024,
                    scratch=sums_of(n),
                )
            else:
                skip = HALO if s == 0 else 0
                own[s], back_rows = call(
                    functools.partial(last_body, skip),
                    (quarters, *parts[s], own[s], other[s], w_step),
                    [((n - skip, width), BF16)] * 2,
                    2 * n * 1024 * 1024,
                )
            if last:
                back.append(lax.ppermute(back_rows, "x", flip))
            else:
                sends[s] = lax.ppermute(partial[s][1], "c", swap)
    out = jnp.zeros((tokens, width), BF16)
    place = 0
    for s in range(2):
        out = lax.dynamic_update_slice_in_dim(out, own[s], late * half + place, 0)
        out = lax.dynamic_update_slice_in_dim(out, back[s], (1 - late) * half + place, 0)
        place += own[s].shape[0]
    return out


def solution(mesh):
    fine = Mesh(mesh.devices.reshape(4, 4, 4, 2), ("z", "y", "x", "c"))
    sp, tp = ("z", "y"), ("x", "c")
    in_specs = (P(sp, tp), P(sp), P(), P(None, tp, sp), P(), P(), P(None, sp, tp))
    return jax.shard_map(layers_body, mesh=fine, in_specs=in_specs, out_specs=P(sp, tp), check_vma=False)
```

```python
import functools

import jax
import jax.numpy as jnp
from jax import lax
from jax.experimental import pallas as pl
from jax.experimental.pallas import tpu as pltpu
from jax.sharding import Mesh, PartitionSpec as P


epsilon = 1e-06
HALO = 64
TAIL = 16
EXTRA = 16
PIECES = 1
VMEM_LIMIT = 16 * 1024 * 1024
LANES = 1024
SEQ = ("z", "y")
F32 = jnp.float32
BF16 = jnp.bfloat16


def nt_dot(a, b):
    return lax.dot_general(a, b, (((1,), (1,)), ((), ())), preferred_element_type=F32)


def dot(a, b):
    return jnp.dot(a, b, preferred_element_type=F32)


def quarter_of(weight, index, k):
    return weight[pl.ds(index[k] * 4, 4)].reshape(256, weight.shape[2])


def call(kernel, operands, shapes, flops, scalars=True, scratch=()):
    memory = pl.BlockSpec(memory_space=pltpu.VMEM)
    specs = [memory] * len(operands)
    if scalars:
        specs[0] = pl.BlockSpec(memory_space=pltpu.SMEM)
    return pl.pallas_call(
        kernel,
        in_specs=specs,
        out_specs=[memory] * len(shapes),
        out_shape=[jax.ShapeDtypeStruct(s, t) for s, t in shapes],
        scratch_shapes=list(scratch),
        compiler_params=pltpu.CompilerParams(vmem_limit_bytes=VMEM_LIMIT),
        cost_estimate=pl.CostEstimate(flops=flops, bytes_accessed=1024, transcendentals=0),
    )(*operands)


def packed(total, lanes):
    high = total.astype(BF16).astype(F32)
    low = total - high
    count = LANES // lanes
    row = lax.broadcasted_iota(jnp.int32, (EXTRA, lanes), 0)
    out = jnp.zeros((EXTRA, lanes), F32)
    for i in range(count):
        cols = slice(i * lanes, (i + 1) * lanes)
        out = jnp.where(row == i, high[:, cols], out)
        out = jnp.where(row == count + i, low[:, cols], out)
    return out.astype(BF16)


def unpacked(block):
    count = LANES // block.shape[1]
    value = block.astype(F32)
    return jnp.concatenate(
        [value[i : i + 1] + value[count + i : count + i + 1] for i in range(count)], axis=1
    )


def square_sums(wide, ones):
    fold = wide * wide
    fold = sum(fold[:, i : i + 128] for i in range(0, fold.shape[1], 128))
    high = fold.astype(BF16)
    low = (fold - high.astype(F32)).astype(BF16)
    return nt_dot(ones, high) + nt_dot(ones, low)


def over_pieces(rows, one):
    size = rows // PIECES
    for i in range(PIECES):
        one(i, slice(i * size, (i + 1) * size))


def project_piece(index, i, here, wide, gain, weights, keep, send, sums):
    sums[i] = square_sums(wide, jnp.ones((8, 128), BF16))
    gained = (wide * gain[...]).astype(BF16)
    for k in range(4):
        columns = jnp.concatenate([quarter_of(weight, index, k) for weight in weights], axis=1)
        part = nt_dot(gained, columns)
        out = keep if k < 2 else send
        out[here, (k % 2) * 256 : (k % 2 + 1) * 256] = part.astype(BF16)


def finish_squares(sums, rows, send, squares):
    parts = [sums[i] for i in range(PIECES)]
    total = jnp.concatenate(parts + [jnp.zeros((8, LANES - rows), F32)], axis=1)[0:1]
    send[rows : rows + EXTRA, :] = packed(total, send.shape[1])
    squares[...] = total


def project_body(index, both, gain, weight, keep, send, squares, sums):
    rows = both.shape[1]

    def turn(half, carry):
        wide = both[half].astype(F32)
        project_piece(
            index, 0, slice(0, rows), wide, gain, (weight,), keep.at[half], send.at[half], sums
        )
        finish_squares(sums, rows, send.at[half], squares.at[half])
        return carry

    lax.fori_loop(0, 2, turn, 0)


def updated(index, here, parts, old, weight):
    total = old[here, :].astype(F32)
    for k, part in enumerate(parts):
        total = total + dot(part[here, :], quarter_of(weight, index, k))
    return total.astype(BF16)


def step_body(
    index, m0, m1, m2, m3, own, other, gain, w0, w1, w2, w3, new_own, new_other, keep, send, squares, sums
):
    def one(i, here):
        first = updated(index, here, (m0, m1, m2, m3), own, w0)
        second = updated(index, here, (m0, m1, m2, m3), other, w1)
        new_own[here, :] = first
        new_other[here, :] = second
        wide = jnp.concatenate([first, second], axis=1).astype(F32)
        project_piece(index, i, here, wide, gain, (w2, w3), keep, send, sums)

    over_pieces(own.shape[0], one)
    finish_squares(sums, own.shape[0], send, squares)


def last_body(skip, index, m0, m1, m2, m3, own, other, w0, w1, out, out_other):
    here = slice(skip, own.shape[0])
    out[...] = updated(index, here, (m0, m1, m2, m3), own, w0)
    out_other[...] = updated(index, here, (m0, m1, m2, m3), other, w1)


def merge_body(keep, core, squares, partner, chip):
    rows = keep.shape[0]
    partner[:rows, :] = (
        keep[:, 256:].astype(F32) + core[:rows, 256:].astype(F32)
    ).astype(BF16)
    total = squares[...] + unpacked(core[rows : rows + EXTRA, :])
    chip[...] = total
    partner[rows : rows + EXTRA, :] = packed(total, 256)


def scatter_body(keep, core, squares, to_pair, to_flip, to_cross, chip):
    rows = keep.shape[1]
    extra = slice(rows, rows + EXTRA)
    totals = [squares[half] + unpacked(core[half, extra, :]) for half in range(2)]
    chip[...] = totals[0]
    for out, half, first in ((to_pair, 0, 256), (to_flip, 1, 256), (to_cross, 1, 0)):
        cols = slice(first, first + 256)
        out[:rows, :] = (
            keep[half, :, cols].astype(F32) + core[half, :rows, cols].astype(F32)
        ).astype(BF16)
        out[extra, :] = packed(totals[half], 256)


def pool_rows(model_width, first, near, far, across, chip, tail, band, share, mix, gain, mixed, new_tail, scales):
    rows = mixed.shape[0]
    total = chip[...]
    for part in across:
        total = total + unpacked(part[rows : rows + EXTRA, :])
    scale = lax.rsqrt(total * (1.0 / model_width) + epsilon)
    for i in range(LANES // 128):
        scales[i] = scale[:, 128 * i : 128 * i + 128]

    def block(i, size, before):
        at = i * 128
        if looped:
            at = pl.multiple_of(at, 128)
        here, there = pl.ds(at, size), pl.ds(first + at, size)
        turned = jnp.transpose(jnp.broadcast_to(scales[i], (128, 128)))[:size]
        summed = near(here).astype(F32) + far(here).astype(F32)
        for part in across:
            summed = summed + part[here, :].astype(F32)
        z = (summed * jnp.concatenate([turned, turned], axis=1)).astype(BF16)
        window = jnp.concatenate([before, z], axis=0)
        for g in range(2):
            cols = slice(g * 128, (g + 1) * 128)
            sums = dot(band[g, there, : size + TAIL], window[:, cols])
            pooled = (sums * share[g, there, :] - z[:, cols].astype(F32)).astype(BF16)
            blended = dot(pooled, mix[g]) * gain[0:1, cols]
            mixed[here, cols] = blended.astype(BF16)
        return z[size - TAIL :]

    whole = rows // 128
    looped = len(across) > 1 or rows % 128 > 0
    before = tail[...]
    if looped:
        before = lax.fori_loop(0, whole, lambda i, carry: block(i, 128, carry), before)
        looped = False
    else:
        for i in range(whole):
            before = block(i, 128, before)
    if rows > whole * 128:
        before = block(whole, rows - whole * 128, before)
    new_tail[...] = before


def pool_body(model_width, first, near, far, across, *rest):
    pool_rows(
        model_width, first, lambda r: near[r, :256], lambda r: far[r, :256], (across,), *rest
    )


def pool_first_body(model_width, first, near, far, across, flipped, crossed, *rest):
    pool_rows(
        model_width,
        first,
        lambda r: near[0, r, :256],
        lambda r: far[0, r, :256],
        (across, flipped, crossed),
        *rest,
    )


def prepare_body(proj_in, proj_out, opening, mine):
    size = proj_in.shape[2]
    row = lax.broadcasted_iota(jnp.int32, (size, size), 0)
    eye = (row == lax.broadcasted_iota(jnp.int32, (size, size), 1)).astype(BF16)
    opening[...] = nt_dot(eye, proj_in[0]).astype(BF16)
    layers = proj_in.shape[0]
    for layer in range(layers):
        mine[2 * layer] = proj_out[layer]
        if layer + 1 < layers:
            mine[2 * layer + 1] = nt_dot(eye, proj_in[layer + 1]).astype(BF16)


def arrange_body(mine, theirs, out):
    paired = theirs.shape[0]
    for i in range(paired):
        out[2 * i] = mine[i]
        out[2 * i + 1] = theirs[i]
    for i in range(paired, mine.shape[0]):
        out[paired + i] = mine[i]


def along_sequence(value, count):
    return lax.ppermute(value, SEQ, [(i, i + 1) for i in range(count - 1)])


def membership(padded, start, rows, group):
    blocks = -(-rows // 128)
    padded = jnp.pad(padded, (0, 128), constant_values=-1)
    sources = jnp.stack(
        [padded[start + 128 * b : start + 128 * b + 128 + TAIL] for b in range(blocks)]
    )
    targets = padded[start + TAIL : start + TAIL + 128 * blocks].reshape(blocks, 128, 1)
    delta = (
        lax.broadcasted_iota(jnp.int32, (128, 128 + TAIL), 0)
        + TAIL
        - lax.broadcasted_iota(jnp.int32, (128, 128 + TAIL), 1)
    )
    member = (sources[:, None, :] == targets) & (delta >= 0)[None]
    bands, shares = [], []
    for g in range(2):
        window = jnp.left_shift(2, (group + g) % 4)
        band = (member & (delta < window)[None]).reshape(blocks * 128, -1)[:rows]
        count = jnp.sum(band.astype(F32), axis=1, keepdims=True)
        bands.append(band.astype(BF16))
        shares.append(jnp.broadcast_to(1.0 / count, (rows, 128)))
    return jnp.stack(bands), jnp.stack(shares)


def layers_body(stream, doc_ids, norm_gain, proj_in, mix_pool, pool_gain, proj_out):
    layers = proj_in.shape[0]
    tokens, width = stream.shape
    model_width = norm_gain.shape[1]
    places = lax.axis_size(SEQ)
    x, c = lax.axis_index("x"), lax.axis_index("c")
    late, p = x // 2, x % 2
    flip = [(i, 3 - i) for i in range(4)]
    pair = [(i, i ^ 1) for i in range(4)]
    swap = [(0, 1), (1, 0)]
    half = tokens // 2
    rows = half + HALO
    split = half // 2
    streams = [(0, split), (split, rows)]

    shard = (proj_in.shape[2], width)
    opening, mine = call(
        prepare_body,
        (proj_in, proj_out),
        [(shard, BF16), ((2 * layers - 1, *shard), BF16)],
        1024,
        scalars=False,
    )

    def spread(shards):
        return jnp.broadcast_to(shards[None], (places, *shards.shape))

    def everyone(copies):
        return lax.all_to_all(copies, SEQ, 0, 0, tiled=True)

    labels_of = (doc_ids + 1).astype(jnp.int32)
    marks = jnp.pad(
        labels_of[-HALO:].astype(BF16)[None], ((0, EXTRA - 1), (0, width - HALO))
    )
    lead = along_sequence(jnp.concatenate([stream[-HALO:], marks]), places)
    w_first = everyone(spread(opening))
    lead_labels = lead[HALO, :HALO].astype(jnp.int32)
    lead = lead[:HALO]
    middle = stream[half - HALO : half]
    middle_labels = labels_of[half - HALO : half]
    own_lead = jnp.where(late == 1, middle, lead)
    other_lead = jnp.where(late == 1, lead, middle)
    labels = jnp.concatenate(
        [
            jnp.where(late == 1, middle_labels, lead_labels),
            lax.dynamic_slice_in_dim(labels_of, late * half, half),
        ]
    )

    def rows_at(side, s):
        lo, hi = max(0, streams[s][0] - HALO), streams[s][1] - HALO
        return lax.dynamic_slice_in_dim(stream, side * half + lo, hi - lo)

    own = [jnp.concatenate([own_lead, rows_at(late, 0)]), rows_at(late, 1)]
    away = [jnp.concatenate([other_lead, rows_at(1 - late, 0)]), rows_at(1 - late, 1)]
    theirs = lax.ppermute(mine[:3], "x", flip)
    other = []
    for s in range(2):
        other.append(lax.ppermute(away[s], "x", flip))
    arranged = call(arrange_body, (mine, theirs), [((8, *shard), BF16)], 1024, scalars=False)[0]
    w_rest = lax.all_gather(arranged, SEQ, axis=0, tiled=False)

    quarters = jnp.stack([2 * c + p, 2 * c + 1 - p, 2 * (1 - c) + p, 2 * (1 - c) + 1 - p]).astype(
        jnp.int32
    )
    group = 2 * (2 * c + p)
    padded = jnp.pad(labels, (TAIL, 0), constant_values=-1)
    band, share = membership(padded, 0, rows, group)

    here, there = (x * 2 + c) * width, ((3 - x) * 2 + c) * width

    def gain_of(layer):
        return jnp.concatenate(
            [lax.dynamic_slice_in_dim(norm_gain[layer], at, width) for at in (here, there)]
        ).astype(F32)[None]

    def sent_shapes(n):
        return [((n, 512), BF16), ((n + EXTRA, 512), BF16), ((1, LANES), F32)]

    def sums_of(n):
        return [pltpu.VMEM((PIECES, 8, n // PIECES), F32)]

    gains = [gain_of(layer) for layer in range(layers)]
    partial, sends = [], []
    for s, (lo, hi) in enumerate(streams):
        n = hi - lo
        partial.append(
            call(
                project_body,
                (quarters, jnp.stack([own[s], away[s]]), gains[0][:, :width], w_first),
                [((2, *shape), kind) for shape, kind in sent_shapes(n)],
                2 * n * 1024 * 1024,
                scratch=sums_of(n),
            )
        )
        sends.append(lax.ppermute(partial[s][1], "c", swap))
    cross = [(i, (i + 2) % 4) for i in range(4)]
    for layer in range(layers):
        mix = lax.dynamic_slice_in_dim(mix_pool[layer], group, 2, 0)
        scale = lax.dynamic_slice_in_dim(pool_gain[layer], group * 128, 256).astype(F32)[None]
        last = layer + 1 == layers
        if layer == 0:
            *w_step, in_own = [w_rest[:, i] for i in (0, 1, 2, 3, 6)]
            in_flipped = lax.ppermute(in_own, "x", flip)
        elif layer == 1:
            w_step = [*later[:2], in_own, in_flipped]
        else:
            w_step = [later[2], out_flipped]
        tail = jnp.zeros((TAIL, 256), BF16)
        merged, parts, back = [], [], []
        for s, (lo, hi) in enumerate(streams):
            n = hi - lo
            keep, _, squares = partial[s]
            message = ((n + EXTRA, 256), BF16)
            routes = (pair, flip, cross) if layer == 0 else (pair,)
            *messages, chip = call(
                scatter_body if layer == 0 else merge_body,
                (keep, sends[s], squares),
                [message] * len(routes) + [((1, LANES), F32)],
                n * 256,
                scalars=False,
            )
            across = [lax.ppermute(value, "x", route) for value, route in zip(messages, routes)]
            merged.append((keep, sends[s], *across, chip))
        for s, (lo, hi) in enumerate(streams):
            n = hi - lo
            mixed, tail = call(
                functools.partial(pool_first_body if layer == 0 else pool_body, model_width, lo),
                (*merged[s], tail, band, share, mix, scale),
                [((n, 256), BF16), ((TAIL, 256), BF16)],
                2 * n * 256 * 1024,
                scalars=False,
                scratch=[pltpu.VMEM((LANES // 128, 1, 128), F32)],
            )
            from_core = lax.ppermute(mixed, "c", swap)
            from_pair = lax.ppermute(mixed, "x", pair)
            from_both = lax.ppermute(from_pair, "c", swap)
            parts.append((mixed, from_pair, from_core, from_both))
        for s, (lo, hi) in enumerate(streams):
            n = hi - lo
            if not last:
                own[s], other[s], *partial[s] = call(
                    step_body,
                    (quarters, *parts[s], own[s], other[s], gains[layer + 1], *w_step),
                    [((n, width), BF16)] * 2 + sent_shapes(n),
                    4 * n * 1024 * 1024,
                    scratch=sums_of(n),
                )
            else:
                skip = HALO if s == 0 else 0
                own[s], back_rows = call(
                    functools.partial(last_body, skip),
                    (quarters, *parts[s], own[s], other[s], *w_step),
                    [((n - skip, width), BF16)] * 2,
                    2 * n * 1024 * 1024,
                )
            if layer + s == 0:
                w_rest, own[0] = lax.optimization_barrier((w_rest, own[0]))
                later = [w_rest[:, i] for i in (4, 5, 7)]
                out_flipped = lax.ppermute(later[2], "x", flip)
            if last:
                back.append(lax.ppermute(back_rows, "x", flip))
            else:
                sends[s] = lax.ppermute(partial[s][1], "c", swap)
    out = jnp.zeros((tokens, width), BF16)
    place = 0
    for s in range(2):
        out = lax.dynamic_update_slice_in_dim(out, own[s], late * half + place, 0)
        out = lax.dynamic_update_slice_in_dim(out, back[s], (1 - late) * half + place, 0)
        place += own[s].shape[0]
    return out


def solution(mesh):
    fine = Mesh(mesh.devices.reshape(4, 4, 4, 2), ("z", "y", "x", "c"))
    sp, tp = ("z", "y"), ("x", "c")
    in_specs = (P(sp, tp), P(sp), P(), P(None, tp, sp), P(), P(), P(None, sp, tp))
    return jax.shard_map(layers_body, mesh=fine, in_specs=in_specs, out_specs=P(sp, tp), check_vma=False)
```
